512 devices in a mesh: fs: 64 (over z, y), tp: 8 (over x, core).
Axes of the slice: x: 4, y: 8, z: 8, core: 2. Of those that a mesh axis runs over, the one named last changes fastest.
Arguments:
- tokens: bfloat16 [8192, 2048], P('fs'), may hold values from -6 to 6
- norm_gain: float32 [2048], replicated, may hold values from 0.1 to 1.9
- w_query: bfloat16 [2048, 1024], P('fs', 'tp'), may hold values from -0.125 to 0.125
- w_key: bfloat16 [2048, 1024], P('fs', 'tp'), may hold values from -0.125 to 0.125
- w_value: bfloat16 [2048, 2048], P('fs', 'tp'), may hold values from -0.125 to 0.125
- w_gate: bfloat16 [2048, 2048], P('fs', 'tp'), may hold values from -0.125 to 0.125
- mixer_gain: float32 [2048], P('tp'), may hold values from 0.1 to 1.9
- w_out: bfloat16 [2048, 2048], P('tp', 'fs'), may hold values from -0.125 to 0.125
- channel_gain: float32 [2048], replicated, may hold values from 0.1 to 1.9
- w_left: bfloat16 [2048, 3072], P('fs', 'tp'), may hold values from -0.125 to 0.125
- w_right: bfloat16 [2048, 3072], P('fs', 'tp'), may hold values from -0.125 to 0.125
- taps_left: float32 [3, 3072], P(None, 'tp'), may hold values from -3.5 to 3.5
- taps_right: float32 [3, 3072], P(None, 'tp'), may hold values from -3.5 to 3.5
- w_down: bfloat16 [3072, 2048], P('tp', 'fs'), may hold values from -0.109375 to 0.109375
Outputs:
- layer_out: bfloat16 [8192, 2048], P('fs')
The draws below stay inside these ranges and needn't reach their ends.
All inputs are finite; a program needn't handle non-finite values.
Results may differ from the reference program's by a relative error of at most 0.018.
Values may be sent and summed in bfloat16 or wider, within the bound.
No kernel may reach another device: no remote copies, remote signals or barrier semaphores. Data moves between devices by JAX's collectives and lax.ppermute only.
A program may use at most 64 MiB of HBM per device.

```python
import jax
import jax.numpy as jnp
from jax import lax

D = 2048
HEADS = 8
DK = 128
DV = 256
FF = 3072
BLOCK = 128
SEQ_LEN = 128
QW = 1024
VW = 2048
TOKENS = 8192
N_TP = 8


def shard_levels(key, shape, pieces, least, top_value):
    level = 1.0
    for axis_at, shards_of in pieces:
        heights = jax.random.uniform(jax.random.fold_in(jax.random.fold_in(key, 6), axis_at), (shards_of,), jnp.float32, least / len(pieces), top_value / len(pieces))
        level = level * jnp.repeat(jnp.exp(heights), shape[axis_at] // shards_of).reshape((-1,) + (1,) * (len(shape) - 1 - axis_at))
    return level


def normal_values(own_key, dims, spread, most, shards=(), held_as=jnp.bfloat16):
    level = shard_levels(own_key, dims, shards, -0.22, 0.18) if shards else 1.0
    drawn = jax.random.normal(own_key, dims, jnp.float32) * spread * level
    return jnp.minimum(jnp.maximum(drawn, -most), most).astype(held_as)


def setup_inputs(seed: int = 0) -> dict:
    keys = jax.random.split(jax.random.key(seed), 15)
    tokens = normal_values(keys[0], (TOKENS, D), 1.0, 6.0, ((0, 64),))
    norm_gain = jnp.clip(1.0 + 0.18 * jax.random.normal(keys[1], (D,), jnp.float32), 0.1, 1.9)
    w_query = normal_values(keys[2], (D, QW), D ** -0.5, 0.125, ((0, 64), (1, 8)))
    w_key = normal_values(keys[3], (D, QW), D ** -0.5, 0.125, ((0, 64), (1, 8)))
    w_value = normal_values(keys[4], (D, VW), D ** -0.5, 0.125, ((0, 64), (1, 8)))
    w_gate = normal_values(keys[5], (D, VW), D ** -0.5, 0.125, ((0, 64), (1, 8)))
    mixer_gain = jnp.clip(1.0 + 0.18 * jax.random.normal(keys[6], (VW,), jnp.float32), 0.1, 1.9)
    w_out = normal_values(keys[7], (VW, D), VW ** -0.5, 0.125, ((0, 8), (1, 64)))
    channel_gain = jnp.clip(1.0 + 0.18 * jax.random.normal(keys[8], (D,), jnp.float32), 0.1, 1.9)
    w_left = normal_values(keys[9], (D, FF), D ** -0.5, 0.125, ((0, 64), (1, 8)))
    w_right = normal_values(keys[10], (D, FF), D ** -0.5, 0.125, ((0, 64), (1, 8)))
    taps_left = normal_values(keys[11], (3, FF), 3 ** -0.5, 3.5, ((1, 8),), jnp.float32)
    taps_right = normal_values(keys[12], (3, FF), 3 ** -0.5, 3.5, ((1, 8),), jnp.float32)
    w_down = normal_values(keys[13], (FF, D), FF ** -0.5, 0.109375, ((0, 8), (1, 64)))
    return dict(tokens=tokens, norm_gain=norm_gain, w_query=w_query, w_key=w_key, w_value=w_value, w_gate=w_gate, mixer_gain=mixer_gain, w_out=w_out, channel_gain=channel_gain, w_left=w_left, w_right=w_right, taps_left=taps_left, taps_right=taps_right, w_down=w_down)


highest = lax.Precision.HIGHEST

def scale_rows(rows_in, gain_vec):
    floats = rows_in.astype(jnp.float32)
    factor = lax.rsqrt(lax.optimization_barrier(jnp.mean(floats * floats, axis=-1, keepdims=True)) + 1e-06)
    return (floats * factor * gain_vec.astype(jnp.float32)).astype(jnp.bfloat16)

def decays(first_head, count):
    head_ids = first_head + jnp.arange(count, dtype=jnp.float32)
    return jnp.log(1.0 - 2.0 ** (-5.0 - head_ids))

def rotate(heads_in, positions):
    width = heads_in.shape[-1]
    half = width // 2
    freqs = 10000.0 ** (-jnp.arange(half, dtype=jnp.float32) / half)
    angles = positions[:, None] * freqs[None, :]
    cosine = jnp.cos(angles)
    sine = jnp.sin(angles)
    first_half = heads_in[..., :half]
    second_half = heads_in[..., half:]
    return jnp.concatenate([first_half * cosine - second_half * sine, first_half * sine + second_half * cosine], axis=-1)

def retention(queries, keys_in, values_in, log_gamma):
    head_count, length, key_width = queries.shape
    value_width = values_in.shape[-1]
    blocks = length // BLOCK
    queries = queries.reshape(head_count, blocks, BLOCK, key_width)
    keys_in = keys_in.reshape(head_count, blocks, BLOCK, key_width)
    values_in = values_in.reshape(head_count, blocks, BLOCK, value_width)
    offsets = jnp.arange(BLOCK, dtype=jnp.float32)
    distance = offsets[:, None] - offsets[None, :]
    weights = jnp.where(distance >= 0, jnp.exp(log_gamma[:, None, None] * jnp.maximum(distance, 0.0)), 0.0)
    scores = jnp.einsum('hbnd,hbmd->hbnm', queries, keys_in, precision=highest) * weights[:, None]
    inner = jnp.einsum('hbnm,hbme->hbne', scores, values_in, precision=highest)
    key_weight = jnp.exp(log_gamma[:, None] * (BLOCK - 1 - offsets)[None, :])
    contrib = jnp.einsum('hbjd,hbje->hbde', keys_in * key_weight[:, None, :, None], values_in, precision=highest)
    block_decay = jnp.exp(log_gamma * BLOCK)[:, None, None]

    def advance(state, contrib_block):
        return (state * block_decay + contrib_block, state)
    _, states = lax.scan(advance, jnp.zeros((head_count, key_width, value_width), jnp.float32), jnp.moveaxis(contrib, 1, 0))
    states = jnp.moveaxis(states, 0, 1)
    query_weight = jnp.exp(log_gamma[:, None] * (offsets + 1.0)[None, :])
    carried = jnp.einsum('hbnd,hbde->hbne', queries, states, precision=highest) * query_weight[:, None, :, None]
    return (inner + carried).reshape(head_count, length, value_width)

def head_norm(retained):
    return retained * lax.rsqrt(lax.optimization_barrier(jnp.mean(retained * retained, axis=-1, keepdims=True)) + 1e-06)

def causal_taps(values_in, taps):
    length = values_in.shape[-2]
    spacing = [(0, 0)] * (values_in.ndim - 2) + [(taps.shape[0] - 1, 0), (0, 0)]
    padded = jnp.pad(values_in.astype(jnp.float32), spacing)
    result = padded[..., 0:length, :] * taps[0]
    for tap_index in range(1, taps.shape[0]):
        result = result + padded[..., tap_index:tap_index + length, :] * taps[tap_index]
    return result

def group_sum(left, weight):
    span = left.shape[1] // N_TP
    running = jnp.zeros((left.shape[0], weight.shape[1]), jnp.float32)
    for group in range(N_TP):
        partial_sum = jnp.dot(left[:, group * span:(group + 1) * span], weight[group * span:(group + 1) * span], preferred_element_type=jnp.float32).astype(jnp.bfloat16)
        running = running + lax.optimization_barrier(partial_sum).astype(jnp.float32)
    return running

def reference(tokens, norm_gain, w_query, w_key, w_value, w_gate, mixer_gain, w_out, channel_gain, w_left, w_right, taps_left, taps_right, w_down):
    seq_count = tokens.shape[0] // SEQ_LEN
    normed = scale_rows(tokens, norm_gain)

    def project(source, weight):
        return jnp.dot(source, weight, preferred_element_type=jnp.float32).astype(jnp.bfloat16)
    queries = project(normed, w_query)
    keys_proj = project(normed, w_key)
    values_proj = project(normed, w_value)
    gates = project(normed, w_gate)
    positions = jnp.arange(SEQ_LEN, dtype=jnp.float32)
    log_gamma = decays(0.0, HEADS)

    def split_heads(rows_in, width):
        return rows_in.astype(jnp.float32).reshape(seq_count, SEQ_LEN, HEADS, width).transpose(0, 2, 1, 3)

    def one_sequence(triple):
        query_heads, key_heads, value_heads = triple
        return head_norm(retention(rotate(query_heads, positions), rotate(key_heads, positions), value_heads, log_gamma))
    retained = lax.map(one_sequence, (split_heads(queries, DK), split_heads(keys_proj, DK), split_heads(values_proj, DV)))
    retained = retained.transpose(0, 2, 1, 3).reshape(seq_count * SEQ_LEN, VW)
    hidden = (retained * mixer_gain * jax.nn.silu(gates.astype(jnp.float32))).astype(jnp.bfloat16)
    middle = (tokens.astype(jnp.float32) + group_sum(hidden, w_out)).astype(jnp.bfloat16)
    normed_mid = scale_rows(middle, channel_gain)
    left = project(normed_mid, w_left)
    right = project(normed_mid, w_right)

    def convolve(rows_in, taps):
        return causal_taps(rows_in.reshape(seq_count, SEQ_LEN, FF), taps).reshape(seq_count * SEQ_LEN, FF)
    gated = (jax.nn.silu(convolve(left, taps_left)) * convolve(right, taps_right)).astype(jnp.bfloat16)
    return (middle.astype(jnp.float32) + group_sum(gated, w_down)).astype(jnp.bfloat16)
```

```python
import functools

import jax
import jax.numpy as jnp
from jax import lax
from jax.experimental import pallas as pl
from jax.experimental.pallas import tpu as pltpu
from jax.sharding import Mesh
from jax.sharding import PartitionSpec as P

DK = 128
DV = 256
FIRST_ROWS = 16
FS = ("zh", "zl", "yh", "yl")
FAR = ("zh", "yh")
NEAR = ("zl", "yl")
TP = ("x", "c")
highest = lax.Precision.HIGHEST


def size_of(axes):
    axes = (axes,) if isinstance(axes, str) else axes
    total = 1
    for name in axes:
        total *= lax.axis_size(name)
    return total


def swap(parts, axes):
    return lax.all_to_all(parts, axes, split_axis=0, concat_axis=0, tiled=True)


def copies_from(x, axes):
    return swap(jnp.broadcast_to(x, (size_of(axes), *x.shape)), axes)


def pack_body(early_count, *refs):
    ins, (early_ref, late_ref) = refs[:-2], refs[-2:]
    early = jnp.concatenate([ref[...] for ref in ins[:early_count]], axis=1)
    for i in range(early_ref.shape[0]):
        early_ref[i] = early
    late_ref[...] = jnp.concatenate([ref[...] for ref in ins[early_count:]], axis=1)


def pack(copies, early, late):
    arrays = [*early, *late]
    rows = arrays[0].shape[0]
    whole = pl.BlockSpec(memory_space=pltpu.VMEM)
    shapes = [
        (copies, rows, sum(a.shape[1] for a in early)),
        (rows, sum(a.shape[1] for a in late)),
    ]
    return pl.pallas_call(
        functools.partial(pack_body, len(early)),
        out_shape=[jax.ShapeDtypeStruct(shape, jnp.bfloat16) for shape in shapes],
        in_specs=[whole] * len(arrays),
        out_specs=[whole] * len(shapes),
    )(*arrays)


def scale_rows(rows_in, gain_vec):
    floats = rows_in.astype(jnp.float32)
    factor = lax.rsqrt(jnp.mean(floats * floats, axis=-1, keepdims=True) + 1e-06)
    return (floats * factor * gain_vec).astype(jnp.bfloat16)


def rotate(rows_in, positions):
    half = rows_in.shape[-1] // 2
    freqs = 10000.0 ** (-jnp.arange(half, dtype=jnp.float32) / half)
    angles = positions[:, None] * freqs[None, :]
    cosine = jnp.cos(angles)
    sine = jnp.sin(angles)
    first_half = rows_in[:, :half]
    second_half = rows_in[:, half:]
    return jnp.concatenate(
        [first_half * cosine - second_half * sine, first_half * sine + second_half * cosine],
        axis=-1,
    )


def retention(queries, keys_in, values_in, log_gamma):
    offsets = jnp.arange(queries.shape[0], dtype=jnp.float32)
    distance = offsets[:, None] - offsets[None, :]
    weights = jnp.where(distance >= 0, jnp.exp(log_gamma * jnp.maximum(distance, 0.0)), 0.0)
    scores = jnp.einsum("nd,md->nm", queries, keys_in, precision=highest) * weights
    return jnp.einsum("nm,me->ne", scores, values_in, precision=highest)


def causal_taps(values_in, taps):
    length = values_in.shape[-2]
    padded = jnp.pad(values_in.astype(jnp.float32), ((taps.shape[0] - 1, 0), (0, 0)))
    result = padded[0:length] * taps[0]
    for tap_index in range(1, taps.shape[0]):
        result = result + padded[tap_index : tap_index + length] * taps[tap_index]
    return result


def dot32(a, b):
    return jnp.dot(a, b, preferred_element_type=jnp.float32)


def near_parts(rows_in):
    rows = rows_in.shape[0]
    far_z, near_z, far_y, near_y = (lax.axis_size(a) for a in FS)
    width = rows_in.shape[1] // (far_z * near_z * far_y * near_y)
    parts = rows_in.reshape(rows, far_z, near_z, far_y, near_y, width)
    parts = parts.transpose(2, 4, 0, 1, 3, 5)
    return parts.reshape(near_z * near_y, rows, far_z * far_y * width)


def from_near_parts(parts):
    far_z, near_z, far_y, near_y = (lax.axis_size(a) for a in FS)
    rows = parts.shape[1]
    width = parts.shape[2] // (far_z * far_y)
    parts = parts.reshape(near_z, near_y, rows, far_z, far_y, width)
    return parts.transpose(2, 3, 0, 4, 1, 5).reshape(rows, -1)


def body(
    tokens,
    norm_gain,
    w_query,
    w_key,
    w_value,
    w_gate,
    mixer_gain,
    w_out,
    channel_gain,
    w_left,
    w_right,
    taps_left,
    taps_right,
    w_down,
):
    length, width = tokens.shape
    near = size_of(NEAR)
    far = size_of(FAR)
    peers = size_of(TP)
    units = w_left.shape[1]

    first, second = pack(
        far, (w_query, w_key, w_value, w_gate, w_out.T), (w_left, w_right, w_down.T)
    )
    late = lax.all_gather(second, FS, axis=0, tiled=True)
    early = swap(first, ("yh", "zh")).reshape(4, 4, w_left.shape[0], -1)
    early = early.transpose(1, 0, 2, 3).reshape(width // near, -1)
    proj_cols = early.shape[1] - DV

    normed = near_parts(scale_rows(tokens, norm_gain))
    me = lax.axis_index(NEAR)
    held = jnp.zeros((near, length, width // near), jnp.bfloat16)
    for d in range(near):
        piece = lax.dynamic_index_in_dim(normed, me ^ d, 0, keepdims=True)
        if d:
            piece = lax.ppermute(piece, NEAR, [(i, i ^ d) for i in range(near)])
        held = lax.dynamic_update_slice_in_dim(held, piece, me ^ d, 0)
    held = held.reshape(near * length, -1)
    part = dot32(held, early[:, :proj_cols]).reshape(near, length, proj_cols)
    fine_part = part[:, :FIRST_ROWS, : 2 * DK]
    fine_part = fine_part - lax.reduce_precision(fine_part, 8, 7)
    middle_bits = lax.reduce_precision(fine_part, 8, 7)
    extra = [middle_bits, fine_part - middle_bits]
    extra.append(jnp.zeros((near, FIRST_ROWS, proj_cols - 4 * DK), jnp.float32))
    part = jnp.concatenate([part, jnp.concatenate(extra, axis=2)], axis=1).astype(jnp.bfloat16)
    part = swap(part, NEAR).astype(jnp.float32)
    total = part[0]
    for d in range(1, near):
        total = total + part[d]
    extra = total[length:, : 2 * DK] + total[length:, 2 * DK : 4 * DK]
    total = total[:length] + jnp.pad(
        extra, ((0, length - FIRST_ROWS), (0, proj_cols - 2 * DK))
    )
    total = lax.reduce_precision(total, 8, 7)
    queries, keys_proj = total[:, :DK], total[:, DK : 2 * DK]
    values_proj, gates = total[:, 2 * DK : 2 * DK + DV], total[:, 2 * DK + DV :]

    head = lax.axis_index(TP).astype(jnp.float32)
    log_gamma = jnp.log(1.0 - 2.0 ** (-5.0 - head))
    positions = jnp.arange(length, dtype=jnp.float32)
    retained = retention(
        rotate(queries, positions), rotate(keys_proj, positions), values_proj, log_gamma
    )
    retained = retained * lax.rsqrt(jnp.mean(retained * retained, axis=-1, keepdims=True) + 1e-06)
    hidden = (retained * mixer_gain * jax.nn.silu(gates)).astype(jnp.bfloat16)

    rows_own = length // peers
    first_row = lax.axis_index(TP) * rows_own
    hidden_near = copies_from(hidden, NEAR).reshape(near * length, DV)
    mixed = lax.dot_general(
        hidden_near,
        early[:, proj_cols:],
        (((1,), (1,)), ((), ())),
        preferred_element_type=jnp.float32,
    ).astype(jnp.bfloat16)
    mixed = mixed.reshape(near * peers // 2, 2, rows_own, -1)
    core = lax.axis_index("c")
    kept = lax.dynamic_index_in_dim(mixed, core, 1, keepdims=False).astype(jnp.float32)
    given = lax.dynamic_index_in_dim(mixed, 1 - core, 1, keepdims=False)
    taken = lax.ppermute(given, "c", [(0, 1), (1, 0)]).astype(jnp.float32)
    arrived = swap((kept + taken).astype(jnp.bfloat16), (*NEAR, "x")).astype(jnp.float32)
    arrived = arrived.reshape(near, peers // 2, rows_own, -1).sum(axis=1)
    residual = lax.dynamic_slice_in_dim(tokens, first_row, rows_own, 0)
    middle_own = (residual.astype(jnp.float32) + from_near_parts(arrived)).astype(jnp.bfloat16)
    normed_mid = lax.all_gather(scale_rows(middle_own, channel_gain), TP, axis=0, tiled=True)

    both = dot32(normed_mid, late[:, : 2 * units]).astype(jnp.bfloat16)
    left, right = both[:, :units], both[:, units:]
    gated = (jax.nn.silu(causal_taps(left, taps_left)) * causal_taps(right, taps_right)).astype(
        jnp.bfloat16
    )
    channel_part = lax.dot_general(
        gated, late[:, 2 * units :], (((1,), (1,)), ((), ())), preferred_element_type=jnp.float32
    ).astype(jnp.bfloat16)
    channel = swap(channel_part.reshape(peers, rows_own, width), TP)
    channel = channel.astype(jnp.float32).sum(axis=0)
    own = (middle_own.astype(jnp.float32) + channel).astype(jnp.bfloat16)
    return lax.all_gather(own, TP, axis=0, tiled=True)


def solution(mesh):
    fs, tp = mesh.devices.shape
    fine = Mesh(mesh.devices.reshape(4, 2, 4, fs // 32, tp // 2, 2), (*FS, *TP))
    placed = (
        P(FS, None),
        P(),
        P(FS, TP),
        P(FS, TP),
        P(FS, TP),
        P(FS, TP),
        P(TP),
        P(TP, FS),
        P(),
        P(FS, TP),
        P(FS, TP),
        P(None, TP),
        P(None, TP),
        P(TP, FS),
    )
    return jax.shard_map(body, mesh=fine, in_specs=placed, out_specs=P(FS, None), check_vma=False)
```
